32 devices in a mesh: ep: 4 (over z), tp: 8 (over y, x, core).
Axes of the slice: x: 2, y: 2, z: 4, core: 2. Of those that a mesh axis runs over, the one named last changes fastest.
Arguments:
- tokens: bfloat16 [512, 2048], P('ep'), may hold values from -6 to 6
- norm_gain: float32 [2048], replicated, may hold values from 0.1 to 1.9
- route_ids: int32 [512, 2], P('ep'), may hold values from 0 to 3, all different within a row; in each aligned block of 128 rows (0 to 127, 128 to 255, ...) at most 96 rows name the same one
- route_weights: float32 [512, 2], P('ep'), may hold values from 0.05 to 1
- gate_proj: bfloat16 [4, 2048, 12288], P('ep', None, 'tp'), may hold values from -0.125 to 0.125
- up_proj: bfloat16 [4, 2048, 12288], P('ep', None, 'tp'), may hold values from -0.125 to 0.125
- down_proj: bfloat16 [4, 12288, 2048], P('ep', 'tp'), may hold values from -0.0546875 to 0.0546875
Outputs:
- mixed: bfloat16 [512, 2048], P('ep', 'tp')
The draws below stay inside these ranges and needn't reach their ends.
Inputs may be any that keep to these rules, and one draw needn't show every extreme that they name: `route_ids`: each token names 2 different experts; within the rows of one device (aligned blocks of 128 tokens) no expert is named by more than 96 pairs, a bound that some block reaches.
All inputs are finite; a program needn't handle non-finite values.
Results may differ from the reference program's by a relative error of at most 0.017.
Values may be sent and summed in bfloat16 or wider, within the bound.
No kernel may reach another device: no remote copies, remote signals or barrier semaphores. Data moves between devices by JAX's collectives and lax.ppermute only.
A program may use at most 64 MiB of HBM per device.

```python
import math
import jax
import jax.numpy as jnp
import numpy as np
from jax import lax

D = 2048
FF = 12288
TOPK = 2
TOK_DEV = 128
EXPERTS = 4
TOKENS = 512
CAP = 96
HID_BLOCK = 1536
N_EP = 4
N_TP = 8


def levels(key, shape, cuts, smallest, largest):
    level, own = 1.0, jax.random.fold_in(key, 6)
    for axis_at, shards_of in cuts:
        draws = jnp.exp(jax.random.uniform(jax.random.fold_in(own, axis_at), (shards_of,), jnp.float32, smallest / len(cuts), largest / len(cuts)))
        level = level * jnp.repeat(draws, shape[axis_at] // shards_of).reshape([-1 if axis == axis_at else 1 for axis in range(len(shape))])
    return level


def assign_block(rng, own, number, rows, count, top, most, skew):
    ranking = jax.random.permutation(rng, count)
    packed, common = shares(count, rows * top, most, skew, True), shares(count, rows * top, most, skew, False)
    places = jnp.arange(count)

    def named(tallies, offset_by):
        used = int((tallies > 0).sum())
        fixed = max(1, used // 4)
        shifted = fixed + (places - fixed + offset_by * (used - fixed)) % max(1, count - fixed)
        return jnp.zeros((count,), jnp.int32).at[ranking[jnp.where(places < fixed, places, shifted)]].set(jnp.asarray(tallies, jnp.int32))

    tallies = jnp.where(number % 4 == 0, named(packed, number // 4), named(common, number - number // 4 - 1))
    mixed = jax.random.permutation(jax.random.fold_in(own, 3), count)
    giver, receiver = mixed[0:count // 2 * 2:2], mixed[1:count // 2 * 2:2]
    slack = jnp.minimum(tallies[giver] - 1, most - tallies[receiver]) // 2
    slack = jnp.where((giver == ranking[0]) | (receiver == ranking[0]) | (tallies[receiver] == 0), 0, jnp.maximum(slack, 0))
    shifted = jax.random.randint(jax.random.fold_in(own, 4), (count // 2,), 0, 1 << 20) % (slack + 1)
    tallies = tallies.at[giver].add(-shifted).at[receiver].add(shifted)
    members = jnp.searchsorted(jnp.cumsum(tallies), jnp.arange(rows * top), side="right").astype(jnp.int32)
    listing = members.reshape(top, rows).T
    listing = listing[jax.random.permutation(jax.random.fold_in(own, 1), rows)]
    offset_by = jax.random.randint(jax.random.fold_in(own, 2), (rows, 1), 0, top)
    return jnp.take_along_axis(listing, (jnp.arange(top)[None, :] + offset_by) % top, axis=1)


def shares(amount, total, limit, slope, full):
    portions = [(1 << 20) // math.isqrt(standing ** slope) + 1 for standing in range(1, amount + 1)]
    largest = limit if full else min(limit, max(-(-total // amount), total * portions[0] // sum(portions)))
    least = 1 if total - largest >= amount - 1 else 0
    holding, rest = [largest] + [least] * (amount - 1), total - largest - least * (amount - 1)
    while rest > 0:
        candidates = [i for i in range(1, amount) if holding[i] < largest] or [i for i in range(1, amount) if holding[i] < limit]
        whole, remaining = sum([portions[i] for i in candidates]), rest
        for i in candidates:
            addition = min(limit - holding[i], max(1, remaining * portions[i] // whole), rest)
            holding[i] = holding[i] + addition
            rest = rest - addition
    return np.array(holding)


def normal_values(key, extent, deviation, most, pieces=(), kind=jnp.bfloat16):
    level = levels(key, extent, pieces, -0.22, 0.18) if pieces else 1.0
    array = jax.random.normal(key, extent, jnp.float32) * deviation * level
    return jnp.minimum(jnp.maximum(array, -most), most).astype(kind)


def setup_inputs(seed: int = 0) -> dict:
    seeds = jax.random.split(jax.random.key(seed), 8)
    tokens = normal_values(seeds[0], (TOKENS, D), 1.0, 6.0, ((0, 4),))
    norm_gain = jnp.clip(1.0 + 0.18 * jax.random.normal(seeds[1], (D,), jnp.float32), 0.1, 1.9)
    route_ids_keys = jax.random.split(jax.random.fold_in(seeds[2], 1), TOKENS // TOK_DEV)
    route_ids_turns = jax.random.permutation(jax.random.fold_in(seeds[2], 3), TOKENS // TOK_DEV)
    route_ids = jax.vmap(lambda own, number: assign_block(jax.random.fold_in(seeds[2], 2), own, number, TOK_DEV, EXPERTS, TOPK, CAP, 2))(route_ids_keys, route_ids_turns).reshape((TOKENS, TOPK))
    route_weights = jnp.clip(jnp.exp(math.log(1.0) - 2.9957323 * jax.random.uniform(seeds[3], (TOKENS, TOPK), jnp.float32) ** levels(seeds[3], (TOKENS, TOPK), ((0, 4),), -0.2, 0.2)), 0.05, 1.0)
    gate_proj = normal_values(seeds[4], (EXPERTS, D, FF), D ** -0.5, 0.125, ((0, 4), (2, 8)))
    up_proj = normal_values(seeds[5], (EXPERTS, D, FF), D ** -0.5, 0.125, ((0, 4), (2, 8)))
    down_proj = normal_values(seeds[6], (EXPERTS, FF, D), FF ** -0.5, 0.0546875, ((0, 4), (1, 8)))
    return dict(tokens=tokens, norm_gain=norm_gain, route_ids=route_ids, route_weights=route_weights, gate_proj=gate_proj, up_proj=up_proj, down_proj=down_proj)


def reference(tokens, norm_gain, route_ids, route_weights, gate_proj, up_proj, down_proj):
    values = tokens.astype(jnp.float32)
    mean_square = lax.optimization_barrier(jnp.mean(values * values, axis=-1, keepdims=True))
    normed = (values * lax.rsqrt(mean_square + 1e-06) * norm_gain).astype(jnp.bfloat16)
    route_flat = route_ids.reshape(N_EP, TOK_DEV * TOPK)
    onehot = (route_flat[:, :, None] == jnp.arange(EXPERTS, dtype=jnp.int32)[None, None, :]).astype(jnp.int32)
    earlier = jnp.cumsum(onehot, axis=1) - onehot
    slot_index = lax.optimization_barrier(jnp.sum(earlier * onehot, axis=-1)).astype(jnp.int32)
    source_ids = jnp.arange(N_EP, dtype=jnp.int32)[:, None]
    buffer_row = (source_ids * CAP + slot_index).reshape(-1)
    expert_ids = route_flat.reshape(-1)
    repeated = jnp.repeat(normed, TOPK, axis=0)
    buffers = jnp.zeros((EXPERTS, N_EP * CAP, D), jnp.bfloat16).at[expert_ids, buffer_row].set(repeated)

    def expert(operands):
        rows_in, gate_w, up_w, down_w = operands
        gate_act = jnp.dot(rows_in, gate_w, preferred_element_type=jnp.float32)
        up_act = jnp.dot(rows_in, up_w, preferred_element_type=jnp.float32)
        hidden = (jax.nn.silu(gate_act) * up_act).astype(jnp.bfloat16)
        hidden_blocks = hidden.reshape(N_EP * CAP, N_TP, HID_BLOCK).astype(jnp.float32)
        down_blocks = down_w.reshape(N_TP, HID_BLOCK, D).astype(jnp.float32)
        partial_value = jnp.einsum('rbf,bfd->brd', hidden_blocks, down_blocks).astype(jnp.bfloat16)
        partial_value = lax.optimization_barrier(partial_value)
        return lax.optimization_barrier(jnp.sum(partial_value.astype(jnp.float32), axis=0))
    results = lax.map(expert, (buffers, gate_proj, up_proj, down_proj))
    picked = results[expert_ids, buffer_row].reshape(TOKENS, TOPK, D)
    mixed = lax.optimization_barrier(jnp.sum(route_weights[:, :, None] * picked, axis=1))
    return mixed.astype(jnp.bfloat16)
```

```python
import jax
import jax.numpy as jnp
from jax import lax
from jax.experimental import pallas as pl
from jax.experimental.pallas import tpu as pltpu
from jax.sharding import PartitionSpec as P


def steps_below(position, size, count):
    total = jnp.zeros_like(position)
    for step in range(1, count):
        total = total + (position >= step * size).astype(jnp.int32)
    return total


def selection(ids, expert, slot, first, second):
    rows = ids.shape[0]
    hit0 = ids[:, 0:1] == expert
    hit1 = ids[:, 1:2] == expert
    member = jnp.where(hit0 | hit1, 1.0, 0.0).astype(jnp.bfloat16)
    earlier = (
        lax.broadcasted_iota(jnp.int32, (rows, rows), 1)
        < lax.broadcasted_iota(jnp.int32, (rows, rows), 0)
    )
    earlier = jnp.where(earlier, 1.0, 0.0).astype(jnp.bfloat16)
    place = jnp.dot(earlier, member, preferred_element_type=jnp.float32)
    here = place == slot.astype(jnp.float32)
    return jnp.where(here & hit0, first, 0.0) + jnp.where(here & hit1, second, 0.0)


def dispatch_kernel(where_ref, tokens_ref, gain_ref, ids_ref, weights_ref, *outs, ep, cap):
    half = cap // 2
    mix_ref, own_ref, sends = outs[0], outs[1], outs[2:]
    mine = where_ref[0]
    core = where_ref[1]
    values = tokens_ref[...].astype(jnp.float32)
    mean_square = jnp.mean(values * values, axis=-1, keepdims=True)
    normed = (values * lax.rsqrt(mean_square + 1e-06) * gain_ref[...]).astype(jnp.bfloat16)
    ids = ids_ref[...]
    weights = weights_ref[...]
    rows = ids.shape[0]

    lanes = cap + (ep - 1) * half
    lane = lax.broadcasted_iota(jnp.int32, (rows, lanes), 1)
    rest = lane - cap
    away = jnp.where(lane < cap, 0, 1 + steps_below(rest, half, ep - 1))
    slot = jnp.where(lane < cap, lane, rest - (away - 1) * half + core * half)
    expert = mine + away
    expert = jnp.where(expert >= ep, expert - ep, expert)
    chosen = selection(ids, expert, slot, 1.0, 1.0).astype(jnp.bfloat16)
    picked = lax.dot_general(
        chosen, normed, (((0,), (0,)), ((), ())), preferred_element_type=jnp.float32
    ).astype(jnp.bfloat16)
    own_ref[...] = picked[:cap]
    for at, send_ref in enumerate(sends):
        send_ref[...] = picked[cap + at * half : cap + (at + 1) * half]

    lane = lax.broadcasted_iota(jnp.int32, (rows, ep * cap), 1)
    away = steps_below(lane, cap, ep)
    expert = mine + away
    expert = jnp.where(expert >= ep, expert - ep, expert)
    mix_ref[...] = selection(ids, expert, lane - away * cap, weights[:, 0:1], weights[:, 1:2])


def down_kernel(where_ref, hidden_ref, down_ref, out_ref):
    out_ref[0] = jnp.dot(
        hidden_ref[...], down_ref[...], preferred_element_type=jnp.float32
    ).astype(out_ref.dtype)


def down_blocks(hidden, down, parity, blocks):
    rows, inner = hidden.shape
    share = down.shape[1] // blocks
    if share % 128:
        whole = lax.dot_general(
            down, hidden, (((0,), (1,)), ((), ())), preferred_element_type=jnp.float32
        )
        whole = whole.astype(jnp.bfloat16).reshape(blocks // 2, 2, share, rows)
        return jnp.swapaxes(lax.dynamic_index_in_dim(whole, parity, 1, keepdims=False), 1, 2)
    return pl.pallas_call(
        down_kernel,
        out_shape=jax.ShapeDtypeStruct((blocks // 2, rows, share), jnp.bfloat16),
        grid_spec=pltpu.PrefetchScalarGridSpec(
            num_scalar_prefetch=1,
            grid=(blocks // 2,),
            in_specs=[
                pl.BlockSpec((rows, inner), lambda i, where: (0, 0)),
                pl.BlockSpec((inner, share), lambda i, where: (0, 2 * i + where[0])),
            ],
            out_specs=pl.BlockSpec((1, rows, share), lambda i, where: (i, 0, 0)),
        ),
        compiler_params=pltpu.CompilerParams(dimension_semantics=("arbitrary",)),
        cost_estimate=pl.CostEstimate(
            flops=rows * inner * down.shape[1],
            bytes_accessed=inner * down.shape[1],
            transcendentals=0,
        ),
    )(parity.reshape(1), hidden, down)


def combine_kernel(mix_ref, *refs):
    out_ref, blocks = refs[-1], refs[:-1]
    cap = blocks[0].shape[0]
    total = None
    for at, block_ref in enumerate(blocks):
        mix = mix_ref[:, at * cap : (at + 1) * cap]
        high = mix.astype(jnp.bfloat16)
        low = (mix - high.astype(jnp.float32)).astype(jnp.bfloat16)
        block = block_ref[...]
        for piece in (high, low):
            term = jnp.dot(piece, block, preferred_element_type=jnp.float32)
            total = term if total is None else total + term
    out_ref[...] = total.astype(out_ref.dtype)


def local(tokens, norm_gain, route_ids, route_weights, gate_proj, up_proj, down_proj):
    ep = lax.axis_size("ep")
    tp = lax.axis_size("tp")
    rows, width = tokens.shape
    topk = route_ids.shape[1]
    cap = min(rows, (3 * rows * topk + 2 * ep - 1) // (2 * ep))
    half = cap // 2
    share = width // tp
    bits = tp.bit_length() - 1
    assert tp == 1 << bits and topk == 2
    at_ep = lax.axis_index("ep").astype(jnp.int32)
    at_tp = lax.axis_index("tp").astype(jnp.int32)
    core = at_tp & 1

    bf16 = jnp.bfloat16
    prepared = pl.pallas_call(
        lambda *refs: dispatch_kernel(*refs, ep=ep, cap=cap),
        out_shape=[
            jax.ShapeDtypeStruct((rows, ep * cap), jnp.float32),
            jax.ShapeDtypeStruct((cap, width), bf16),
        ]
        + [jax.ShapeDtypeStruct((half, width), bf16)] * (ep - 1),
        in_specs=[pl.BlockSpec(memory_space=pltpu.SMEM)]
        + [pl.BlockSpec(memory_space=pltpu.VMEM)] * 4,
    )(jnp.stack([at_ep, core]), tokens, norm_gain.reshape(1, width), route_ids, route_weights)
    mix, own, sends = prepared[0], prepared[1], prepared[2:]

    pairs = [(i, i ^ 1) for i in range(tp)]
    pieces = [own]
    for away, send in enumerate(sends, 1):
        got = lax.ppermute(send, "ep", [(i, (i + away) % ep) for i in range(ep)])
        other = lax.ppermute(got, "tp", pairs)
        pieces += [jnp.where(core == 0, got, other), jnp.where(core == 0, other, got)]
    merged = jnp.concatenate(pieces, axis=0)

    gate = jnp.dot(merged, gate_proj[0], preferred_element_type=jnp.float32)
    up = jnp.dot(merged, up_proj[0], preferred_element_type=jnp.float32)
    hidden = (jax.nn.silu(gate) * up).astype(bf16)

    send = down_blocks(hidden, down_proj[0], 1 - core, tp)
    got = lax.ppermute(send, "tp", pairs)
    keep = down_blocks(hidden, down_proj[0], core, tp)
    count = ep * cap
    total = keep.astype(jnp.float32) + got.astype(jnp.float32)
    total = total.reshape((2,) * (bits - 1) + (count, share))
    axes = tuple(range(bits - 2, -1, -1)) + (bits - 1, bits)
    total = jnp.where(core == 0, jnp.transpose(total, axes), total).astype(bf16)
    for step in range(bits - 1):
        even, odd = 1 + step, bits - 1 - step
        bit = jnp.where(core == 0, at_tp >> even, at_tp >> odd) & 1
        swap = [(i, i ^ (1 << (odd if i & 1 else even))) for i in range(tp)]
        send = lax.dynamic_index_in_dim(total, 1 - bit, 0, keepdims=False)
        keep = lax.dynamic_index_in_dim(total, bit, 0, keepdims=False)
        got = lax.ppermute(send, "tp", swap)
        total = (keep.astype(jnp.float32) + got.astype(jnp.float32)).astype(bf16)

    back = [total[:cap]]
    for away in range(1, ep):
        block = total[away * cap : (away + 1) * cap]
        back.append(lax.ppermute(block, "ep", [(i, (i - away) % ep) for i in range(ep)]))
    return pl.pallas_call(
        combine_kernel,
        out_shape=jax.ShapeDtypeStruct((rows, share), bf16),
        in_specs=[pl.BlockSpec(memory_space=pltpu.VMEM)] * (ep + 1),
    )(mix, *back)


def solution(mesh):
    placed = (
        P("ep", None),
        P(),
        P("ep", None),
        P("ep", None),
        P("ep", None, "tp"),
        P("ep", None, "tp"),
        P("ep", "tp", None),
    )
    return jax.shard_map(
        local, mesh=mesh, in_specs=placed, out_specs=P("ep", "tp"), check_vma=False
    )
```
